32 devices in a mesh: rep: 4 (over z), fs: 4 (over y, x), tp: 2 (over core).
Axes of the slice: x: 2, y: 2, z: 4, core: 2. Of those that a mesh axis runs over, the one named last changes fastest.
Arguments:
- inputs: bfloat16 [4096, 2048], P(('rep', 'fs', 'tp')), may hold values from -6 to 6
- out_grad: bfloat16 [4096, 2048], P(('rep', 'fs', 'tp')), may hold values from -6 to 6
- pre_act: bfloat16 [4096, 8192], P('rep', ('fs', 'tp')), may hold values from -6 to 6
- w_up: bfloat16 [2048, 8192], P('rep', ('fs', 'tp')), may hold values from -0.125 to 0.125
- w_down_t: bfloat16 [2048, 8192], P('rep', ('fs', 'tp')), may hold values from -0.0625 to 0.0625
Outputs:
- grad_in: bfloat16 [4096, 2048], P(('rep', 'fs', 'tp'))
- grad_up: float32 [2048, 8192], P('rep', ('fs', 'tp'))
- grad_down_t: float32 [2048, 8192], P('rep', ('fs', 'tp'))
The draws below stay inside these ranges and needn't reach their ends.
All inputs are finite; a program needn't handle non-finite values.
Results may differ from the reference program's by a relative error of at most 0.014.
Values may be sent and summed in bfloat16 or wider, within the bound.
No kernel may reach another device: no remote copies, remote signals or barrier semaphores. Data moves between devices by JAX's collectives and lax.ppermute only.
A program may use at most 128 MiB of HBM per device.

```python
import jax
import jax.numpy as jnp
from jax import lax

D = 2048
FF = 8192
TOKENS = 4096
N_FS = 4
N_TP = 2


def with_spikes(entries, rng, source, target, shards_of, factor):
    owner, partner = [(jnp.arange(entries.shape[position]) // (entries.shape[position] // shards_of)).reshape([-1 if axis == position else 1 for axis in range(entries.ndim)]) for position in (source, target)]
    chosen = jax.random.permutation(rng, shards_of)[partner]
    strong = (owner == chosen) | (owner == (partner + shards_of // 2) % shards_of)
    return jnp.where(strong, factor * entries, entries)


def shard_levels(own_key, dims, cuts, low, top_value):
    level, own = 1.0, jax.random.fold_in(own_key, 6)
    for dim, shards_of in cuts:
        draws = jnp.exp(jax.random.uniform(jax.random.fold_in(own, dim), (shards_of,), jnp.float32, low / len(cuts), top_value / len(cuts)))
        level = level * jnp.repeat(draws, dims[dim] // shards_of).reshape([-1 if axis == dim else 1 for axis in range(len(dims))])
    return level


def noise(rng, extent, scale, most, cuts=(), dtype=jnp.bfloat16):
    factor_of = shard_levels(rng, extent, cuts, -0.22, 0.18) if cuts else 1.0
    values = jax.random.normal(rng, extent, jnp.float32) * scale * factor_of
    return jnp.minimum(jnp.maximum(values, -most), most).astype(dtype)


def noise_with(own_key, dims, spread, reach, pieces, heavy, kind=jnp.bfloat16):
    result = spread * jax.random.normal(own_key, dims, jnp.float32)
    if pieces:
        result = result * shard_levels(own_key, dims, pieces, -0.22, 0.18)
    return jnp.clip(with_spikes(result, jax.random.fold_in(own_key, 3), *heavy), -reach, reach).astype(kind)


def setup_inputs(seed: int = 0) -> dict:
    arg_keys = jax.random.split(jax.random.key(seed), 6)
    inputs = noise(arg_keys[0], (TOKENS, D), 1.0, 6.0, ((0, 32),))
    out_grad = noise_with(arg_keys[1], (TOKENS, D), 1.0, 6.0, ((0, 32),), (0, 1, 32, 2.75))
    pre_act = noise(arg_keys[2], (TOKENS, FF), 1.0, 6.0, ((0, 4), (1, 8)))
    w_up = noise(arg_keys[3], (D, FF), D ** -0.5, 0.125, ((0, 4), (1, 8)))
    w_down_t = noise(arg_keys[4], (D, FF), FF ** -0.5, 0.0625, ((0, 4), (1, 8)))
    return {"inputs": inputs, "out_grad": out_grad, "pre_act": pre_act, "w_up": w_up, "w_down_t": w_down_t}


def reference(inputs, out_grad, pre_act, w_up, w_down_t):
    pre_float = pre_act.astype(jnp.float32)
    linear = jnp.maximum(pre_float, 0.0)
    squared = (linear * linear).astype(jnp.bfloat16)
    grad_squared = jnp.dot(out_grad, w_down_t, preferred_element_type=jnp.float32)
    grad_pre = (grad_squared * 2.0 * linear).astype(jnp.bfloat16)
    factor = float(TOKENS) ** -0.5
    grad_down_t = jnp.dot(out_grad.T, squared, preferred_element_type=jnp.float32) * factor
    grad_up = jnp.dot(inputs.T, grad_pre, preferred_element_type=jnp.float32) * factor
    blocks = N_FS * N_TP
    width = FF // blocks
    total = jnp.zeros((inputs.shape[0], D), jnp.float32)
    for index in range(blocks):
        term = jnp.dot(grad_pre[:, index * width:(index + 1) * width], w_up[:, index * width:(index + 1) * width].T, preferred_element_type=jnp.float32)
        term = lax.optimization_barrier(term.astype(jnp.bfloat16))
        total = total + term.astype(jnp.float32)
    return total.astype(jnp.bfloat16), grad_up, grad_down_t
```

```python
import jax
import jax.numpy as jnp
from jax import lax
from jax.sharding import PartitionSpec as P


def on_device(inputs, out_grad, pre_act, w_up, w_down_t):
    f32, bf16 = jnp.float32, jnp.bfloat16
    count = lax.axis_size("rep")
    here = lax.axis_index("rep")
    mirror = count - 1 - here
    group = ("fs", "tp")
    rows, cols = w_up.shape
    tokens = pre_act.shape[0]
    factor = float(tokens * count) ** (-0.5)
    forward = [(i, i + 1) for i in range(count - 1)]
    backward = [(i + 1, i) for i in range(count - 1)]

    def shift(up, down):
        return lax.ppermute(up, "rep", forward), lax.ppermute(down, "rep", backward)

    def fence(*values):
        return lax.optimization_barrier(values)

    def store(buffer, own, got, step):
        for value, index, valid in (
            (got[0], here - step, here >= step),
            (got[1], here + step, mirror >= step),
        ):
            block = jnp.where(valid, value, own)
            buffer = lax.dynamic_update_slice(buffer, block, (jnp.where(valid, index, here) * rows, 0))
        return buffer

    def part(sums, index):
        return lax.dynamic_slice(sums, (jnp.clip(index, 0, count - 1) * rows, 0), (rows, cols))

    def payload(got, sums, step):
        away = count - step
        result = []
        for value, index, place in ((got[0], here + away, here), (got[1], here - away, mirror)):
            summed = (value.astype(f32) + part(sums, index).astype(f32)).astype(bf16)
            result.append(jnp.where(place <= step - 1, summed, value))
        return result

    def total(got, sums):
        return got[0].astype(f32) + got[1].astype(f32) + part(sums, here).astype(f32)

    def start(own):
        return lax.dynamic_update_slice(jnp.zeros((count * rows, cols), bf16), own, (here * rows, 0))

    grad_rows = lax.all_gather(out_grad, group, axis=0, tiled=True)
    got_a = shift(w_down_t, w_down_t)
    a0, a1, up_own, inputs_late = fence(*got_a, w_up, inputs)
    input_rows = lax.all_gather(inputs_late, group, axis=0, tiled=True)

    got_b = shift(up_own, up_own)
    linear = jnp.maximum(pre_act.astype(f32), 0.0)
    squared = (linear * linear).astype(bf16)
    down_sums = lax.dot_general(
        grad_rows, squared, (((0,), (0,)), ((), ())), preferred_element_type=f32
    )
    down_sums = (down_sums * factor).astype(bf16)
    b0, b1, a0, a1, down_sums = fence(*got_b, a0, a1, down_sums)

    down_full = store(start(w_down_t), w_down_t, (a0, a1), 1)
    got = (a0, a1)
    for step in range(2, count):
        got = shift(*payload(got, down_sums, step - 1))
        got = fence(*got)
        down_full = store(down_full, w_down_t, got, step)
    last = payload(got, down_sums, count - 1)
    l0, l1, down_full, b0, b1 = fence(*last, down_full, b0, b1)
    got_c = shift(l0, l1)
    grad_squared = jnp.dot(grad_rows, down_full, preferred_element_type=f32)
    grad_pre = (grad_squared * 2.0 * linear).astype(bf16)
    up_sums = lax.dot_general(
        input_rows, grad_pre, (((0,), (0,)), ((), ())), preferred_element_type=f32
    )
    up_sums = (up_sums * factor).astype(bf16)
    c0, c1, b0, b1, grad_pre, up_sums = fence(*got_c, b0, b1, grad_pre, up_sums)
    grad_down_t = total((c0, c1), down_sums)

    def terms(weights):
        product = lax.dot_general(
            grad_pre, weights, (((1,), (1,)), ((), ())), preferred_element_type=f32
        ).astype(bf16)
        return lax.psum_scatter(product, group, scatter_dimension=0, tiled=True)

    low = jnp.maximum(here - 1, 0)
    first = jnp.where(here == 0, up_own, b0)
    second = jnp.where(here == 0, b1, up_own)
    near = terms(jnp.concatenate([first, second], axis=0))
    grad_in = jnp.zeros((near.shape[0], count * rows), bf16)

    up_full = store(start(up_own), up_own, (b0, b1), 1)
    got = (b0, b1)
    for step in range(2, count):
        got = shift(*payload(got, up_sums, step - 1))
        got = fence(*got)
        up_full = store(up_full, up_own, got, step)
    last = payload(got, up_sums, count - 1)
    l0, l1, up_full = fence(*last, up_full)
    got_d = shift(l0, l1)
    grad_in = lax.dynamic_update_slice(grad_in, near, (0, low * rows))
    if count > 2:
        places = [jnp.where(low > t, t, t + 2) for t in range(count - 2)]
        far = terms(jnp.concatenate([part(up_full, place) for place in places], axis=0))
        for t, place in enumerate(places):
            grad_in = lax.dynamic_update_slice(
                grad_in, far[:, t * rows : (t + 1) * rows], (0, place * rows)
            )
    grad_up = total(got_d, up_sums)
    return (grad_in, grad_up, grad_down_t)


def solution(mesh):
    in_specs = (
        P(("rep", "fs", "tp"), None),
        P(("rep", "fs", "tp"), None),
        P("rep", ("fs", "tp")),
        P("rep", ("fs", "tp")),
        P("rep", ("fs", "tp")),
    )
    out_specs = (P(("rep", "fs", "tp"), None), P("rep", ("fs", "tp")), P("rep", ("fs", "tp")))
    return jax.shard_map(
        on_device, mesh=mesh, in_specs=in_specs, out_specs=out_specs, check_vma=False
    )
```
